32 devices in a mesh: ep: 8 (over z, y), tp: 4 (over x, core).
Axes of the slice: x: 2, y: 2, z: 4, core: 2. Of those that a mesh axis runs over, the one named last changes fastest.
Arguments:
- tokens: bfloat16 [512, 1024], P('ep', 'tp'), may hold values from -6 to 6
- conv_state: bfloat16 [512, 3, 512], P('ep', None, 'tp'), may hold values from -6 to 6
- lru_state: float32 [512, 512], P('ep', 'tp'), may hold values from -6 to 6
- mix_gain: bfloat16 [1024], replicated, may hold values from 0.099609375 to 1.8984375
- ffn_gain: bfloat16 [1024], replicated, may hold values from 0.099609375 to 1.8984375
- w_branch: bfloat16 [1024, 512], P(None, 'tp'), may hold values from -0.1875 to 0.1875
- w_gate: bfloat16 [1024, 512], P(None, 'tp'), may hold values from -0.1875 to 0.1875
- conv_taps: bfloat16 [4, 512], P(None, 'tp'), may hold values from -3 to 3
- w_recur: bfloat16 [8, 64, 64], P('tp'), may hold values from -0.75 to 0.75
- w_inject: bfloat16 [8, 64, 64], P('tp'), may hold values from -0.75 to 0.75
- lru_lambda: float32 [512], P('tp'), may hold values from 2 to 7
- w_out: bfloat16 [512, 1024], P('tp'), may hold values from -0.25 to 0.25
- expert_gate: bfloat16 [8, 1024, 2560], P('ep', None, 'tp'), may hold values from -0.1875 to 0.1875
- expert_up: bfloat16 [8, 1024, 2560], P('ep', None, 'tp'), may hold values from -0.1875 to 0.1875
- expert_down: bfloat16 [8, 2560, 1024], P('ep', 'tp'), may hold values from -0.125 to 0.125
- route_ids: int32 [512, 2], P('ep'), may hold values from 0 to 7, all different within a row; in each aligned block of 64 rows (0 to 63, 64 to 127, ...) at most 32 rows name the same one
- route_weight: float32 [512, 2], P('ep'), may hold values from 0.2 to 1
Outputs:
- mixed: bfloat16 [512, 1024], P('ep', 'tp')
- state_out: float32 [512, 512], P('ep', 'tp')
The draws below stay inside these ranges and needn't reach their ends.
Inputs may be any that keep to these rules, and one draw needn't show every extreme that they name: `route_ids`: each row names 2 different experts. Among the 64 rows of one device no expert is named more than 32 times, and in every draw some expert is named exactly 32 times by them.
All inputs are finite; a program needn't handle non-finite values.
Results may differ from the reference program's by a relative error of at most 0.015.
Values may be sent and summed in bfloat16 or wider, within the bound.
A program may use at most 64 MiB of HBM per device.

```python
import math
import jax
import jax.numpy as jnp
import numpy as np
from jax import lax

D = 1024
HEADS = 8
HEAD_W = 64
W_A = 512
CONV = 4
FF = 2560
SEQS = 64
TOP = 2
EXPERTS = 8
CAP = 32
SEQ_ALL = 512
N_TP = 4


def block_levels(stream_key, dims, shards, smallest, largest):
    loudness = 1.0
    for axis_at, shards_of in shards:
        heights = jax.random.uniform(jax.random.fold_in(jax.random.fold_in(stream_key, 6), axis_at), (shards_of,), jnp.float32, smallest / len(shards), largest / len(shards))
        loudness = loudness * jnp.repeat(jnp.exp(heights), dims[axis_at] // shards_of).reshape((-1,) + (1,) * (len(dims) - 1 - axis_at))
    return loudness


def routed_block(rng, own, number, rows, number_of, top, reach, skew):
    ranking = jax.random.permutation(rng, number_of)
    packed, usual = shares(number_of, rows * top, reach, skew, True), shares(number_of, rows * top, reach, skew, False)
    places = jnp.arange(number_of)

    def named(tallies, rotation):
        used = int((tallies > 0).sum())
        fixed = max(1, used // 4)
        moved = fixed + (places - fixed + rotation * (used - fixed)) % max(1, number_of - fixed)
        return jnp.zeros((number_of,), jnp.int32).at[ranking[jnp.where(places < fixed, places, moved)]].set(jnp.asarray(tallies, jnp.int32))

    tallies = jnp.where(number % 4 == 0, named(packed, number // 4), named(usual, number - number // 4 - 1))
    mixed = jax.random.permutation(jax.random.fold_in(own, 3), number_of)
    donor, sink = mixed[0:number_of // 2 * 2:2], mixed[1:number_of // 2 * 2:2]
    slack = jnp.minimum(tallies[donor] - 1, reach - tallies[sink]) // 2
    slack = jnp.where((donor == ranking[0]) | (sink == ranking[0]) | (tallies[sink] == 0), 0, jnp.maximum(slack, 0))
    moved = jax.random.randint(jax.random.fold_in(own, 4), (number_of // 2,), 0, 1 << 20) % (slack + 1)
    tallies = tallies.at[donor].add(-moved).at[sink].add(moved)
    items = jnp.searchsorted(jnp.cumsum(tallies), jnp.arange(rows * top), side="right").astype(jnp.int32)
    table = items.reshape(top, rows).T
    table = table[jax.random.permutation(jax.random.fold_in(own, 1), rows)]
    rotation = jax.random.randint(jax.random.fold_in(own, 2), (rows, 1), 0, top)
    return jnp.take_along_axis(table, (jnp.arange(top)[None, :] + rotation) % top, axis=1)


def shares(count, total, reach, skew, full):
    loads = [(1 << 20) // math.isqrt(grade ** skew) + 1 for grade in range(1, count + 1)]
    largest = reach if full else min(reach, max(-(-total // count), total * loads[0] // sum(loads)))
    least = 1 if total - largest >= count - 1 else 0
    given, surplus = [largest] + [least] * (count - 1), total - largest - least * (count - 1)
    while surplus > 0:
        candidates = [i for i in range(1, count) if given[i] < largest] or [i for i in range(1, count) if given[i] < reach]
        whole, remaining = sum([loads[i] for i in candidates]), surplus
        for i in candidates:
            extra = min(reach - given[i], max(1, remaining * loads[i] // whole), surplus)
            given[i] = given[i] + extra
            surplus = surplus - extra
    return np.array(given)


def gaussian(stream_key, dims, spread, limit, pieces=(), kind=jnp.bfloat16):
    factor_of = block_levels(stream_key, dims, pieces, -0.22, 0.18) if pieces else 1.0
    result = jax.random.normal(stream_key, dims, jnp.float32) * spread * factor_of
    return jnp.minimum(jnp.maximum(result, -limit), limit).astype(kind)


def setup_inputs(seed: int = 0) -> dict:
    splits = jax.random.split(jax.random.key(seed), 18)
    tokens = gaussian(splits[0], (SEQ_ALL, D), 1.0, 6.0, ((0, 8), (1, 4)))
    conv_state = gaussian(splits[1], (SEQ_ALL, CONV - 1, W_A), 1.0, 6.0, ((0, 8), (2, 4)))
    lru_state = gaussian(splits[2], (SEQ_ALL, W_A), 1.0, 6.0, ((0, 8), (1, 4)), jnp.float32)
    mix_gain = jnp.clip(1.0 + 0.18 * jax.random.normal(splits[3], (D,), jnp.float32), 0.099609375, 1.8984375).astype(jnp.bfloat16)
    ffn_gain = jnp.clip(1.0 + 0.18 * jax.random.normal(splits[4], (D,), jnp.float32), 0.099609375, 1.8984375).astype(jnp.bfloat16)
    w_branch = gaussian(splits[5], (D, W_A), D ** -0.5, 0.1875, ((1, 4),))
    w_gate = gaussian(splits[6], (D, W_A), D ** -0.5, 0.1875, ((1, 4),))
    conv_taps = gaussian(splits[7], (CONV, W_A), 0.5, 3.0, ((1, 4),))
    w_recur = gaussian(splits[8], (HEADS, HEAD_W, HEAD_W), HEAD_W ** -0.5, 0.75, ((0, 4),))
    w_inject = gaussian(splits[9], (HEADS, HEAD_W, HEAD_W), HEAD_W ** -0.5, 0.75, ((0, 4),))
    lru_lambda = jnp.clip(2.0 + 5.0 * jax.random.uniform(splits[10], (W_A,), jnp.float32) ** block_levels(splits[10], (W_A,), ((0, 4),), -0.2, 0.2), 2.0, 7.0)
    w_out = gaussian(splits[11], (W_A, D), W_A ** -0.5, 0.25, ((0, 4),))
    expert_gate = gaussian(splits[12], (EXPERTS, D, FF), D ** -0.5, 0.1875, ((0, 8), (2, 4)))
    expert_up = gaussian(splits[13], (EXPERTS, D, FF), D ** -0.5, 0.1875, ((0, 8), (2, 4)))
    expert_down = gaussian(splits[14], (EXPERTS, FF, D), FF ** -0.5, 0.125, ((0, 8), (1, 4)))
    route_ids_keys = jax.random.split(jax.random.fold_in(splits[15], 1), SEQ_ALL // SEQS)
    route_ids_turns = jax.random.permutation(jax.random.fold_in(splits[15], 3), SEQ_ALL // SEQS)
    route_ids = jax.vmap(lambda own, number: routed_block(jax.random.fold_in(splits[15], 2), own, number, SEQS, EXPERTS, TOP, CAP, 2))(route_ids_keys, route_ids_turns).reshape((SEQ_ALL, TOP))
    route_weight = jnp.clip(0.2 + 0.8 * jax.random.uniform(splits[16], (SEQ_ALL, TOP), jnp.float32) ** block_levels(splits[16], (SEQ_ALL, TOP), ((0, 8),), -0.2, 0.2), 0.2, 1.0)
    return {"tokens": tokens, "conv_state": conv_state, "lru_state": lru_state, "mix_gain": mix_gain, "ffn_gain": ffn_gain, "w_branch": w_branch, "w_gate": w_gate, "conv_taps": conv_taps, "w_recur": w_recur, "w_inject": w_inject, "lru_lambda": lru_lambda, "w_out": w_out, "expert_gate": expert_gate, "expert_up": expert_up, "expert_down": expert_down, "route_ids": route_ids, "route_weight": route_weight}


EPS = 1e-06
LRU_SCALE = 8.0

def rms_rows(rows, gain):
    values = rows.astype(jnp.float32)
    scaled = values * lax.rsqrt(lax.optimization_barrier(jnp.mean(values * values, axis=-1, keepdims=True)) + EPS)
    return (scaled * gain.astype(jnp.float32)).astype(jnp.bfloat16)

def split_sum(left, right, groups):
    count = left.shape[0]
    width = left.shape[1] // groups
    parts = jnp.einsum('ngk,gkm->ngm', left.reshape(count, groups, width).astype(jnp.float32), right.reshape(groups, width, right.shape[1]).astype(jnp.float32))
    rounded = lax.optimization_barrier(parts.astype(jnp.bfloat16)).astype(jnp.float32)
    return lax.optimization_barrier(jnp.sum(rounded, axis=1)).astype(jnp.bfloat16)

def reference(tokens, conv_state, lru_state, mix_gain, ffn_gain, w_branch, w_gate, conv_taps, w_recur, w_inject, lru_lambda, w_out, expert_gate, expert_up, expert_down, route_ids, route_weight):
    count = tokens.shape[0]
    normed = rms_rows(tokens, mix_gain)
    branch = jnp.dot(normed, w_branch, preferred_element_type=jnp.float32).astype(jnp.bfloat16)
    gate_in = jnp.dot(normed, w_gate, preferred_element_type=jnp.float32).astype(jnp.bfloat16)
    window = jnp.concatenate([conv_state, branch[:, None, :]], axis=1).astype(jnp.float32)
    conv_out = lax.optimization_barrier(jnp.sum(window * conv_taps.astype(jnp.float32)[None], axis=1))
    conv_heads = lax.optimization_barrier(conv_out.astype(jnp.bfloat16)).astype(jnp.float32).reshape(count, HEADS, HEAD_W)
    recur = jax.nn.sigmoid(jnp.einsum('nhi,hij->nhj', conv_heads, w_recur.astype(jnp.float32)).reshape(count, HEADS * HEAD_W))
    inject = jax.nn.sigmoid(jnp.einsum('nhi,hij->nhj', conv_heads, w_inject.astype(jnp.float32)).reshape(count, HEADS * HEAD_W))
    log_decay = -LRU_SCALE * recur * jax.nn.softplus(-lru_lambda)
    state_out = jnp.exp(log_decay) * lru_state + jnp.sqrt(-jnp.expm1(2.0 * log_decay)) * inject * conv_out
    lru_out = (state_out * jax.nn.gelu(gate_in.astype(jnp.float32))).astype(jnp.bfloat16)
    mix_out = split_sum(lru_out, w_out, N_TP)
    resid = (tokens.astype(jnp.float32) + mix_out.astype(jnp.float32)).astype(jnp.bfloat16)
    normed2 = rms_rows(resid, ffn_gain)
    groups = count // SEQS
    flat = route_ids.reshape(groups, SEQS * TOP).astype(jnp.int32)
    onehot = (flat[:, :, None] == jnp.arange(EXPERTS, dtype=jnp.int32)[None, None, :]).astype(jnp.int32)
    before = jnp.cumsum(onehot, axis=1) - onehot
    slot = lax.optimization_barrier(jnp.sum(before * onehot, axis=2)).astype(jnp.int32)
    where = (jnp.arange(groups, dtype=jnp.int32)[:, None] * CAP + slot).reshape(-1).astype(jnp.int32)
    token_of = (jnp.arange(groups, dtype=jnp.int32)[:, None] * SEQS + jnp.arange(SEQS * TOP, dtype=jnp.int32)[None, :] // TOP).reshape(-1).astype(jnp.int32)
    expert_of = flat.reshape(-1)
    table = jnp.full((EXPERTS, groups * CAP), count, jnp.int32).at[expert_of, where].set(token_of)
    padded = jnp.concatenate([normed2, jnp.zeros((1, D), jnp.bfloat16)], axis=0)

    def one_expert(args):
        rows_idx, e_gate, e_up, e_down = args
        rows = padded[rows_idx].astype(jnp.float32)
        first = jnp.dot(rows, e_gate.astype(jnp.float32))
        second = jnp.dot(rows, e_up.astype(jnp.float32))
        hidden = (jax.nn.silu(first) * second).astype(jnp.bfloat16)
        return split_sum(hidden, e_down, N_TP)
    outputs = lax.map(one_expert, (table, expert_gate, expert_up, expert_down))
    picked = outputs[expert_of, where].reshape(count, TOP, D).astype(jnp.float32)
    moe = lax.optimization_barrier(jnp.sum(picked * route_weight[:, :, None], axis=1))
    mixed = (resid.astype(jnp.float32) + moe).astype(jnp.bfloat16)
    return (mixed, state_out)
```

```python
import functools

import jax
import jax.numpy as jnp
from jax import lax
from jax.experimental import pallas as pl
from jax.experimental.pallas import tpu as pltpu
from jax.sharding import PartitionSpec as P

D = 1024


EPS = 1e-06
LRU_SCALE = 8.0


def rms_rows(rows, gain):
    values = rows.astype(jnp.float32)
    scaled = values * lax.rsqrt(jnp.mean(values * values, axis=-1, keepdims=True) + EPS)
    return (scaled * gain.astype(jnp.float32)).astype(jnp.bfloat16)


def body(
    tokens,
    conv_state,
    lru_state,
    mix_gain,
    ffn_gain,
    w_branch,
    w_gate,
    conv_taps,
    w_recur,
    w_inject,
    lru_lambda,
    w_out,
    expert_gate,
    expert_up,
    expert_down,
    route_ids,
    route_weight,
):
    seqs = tokens.shape[0]
    whole = lax.all_gather(tokens, "tp", axis=1, tiled=True)
    normed = rms_rows(whole, mix_gain)
    branch = jnp.dot(normed, w_branch, preferred_element_type=jnp.float32).astype(jnp.bfloat16)
    gate_in = jnp.dot(normed, w_gate, preferred_element_type=jnp.float32).astype(jnp.bfloat16)
    window = jnp.concatenate([conv_state, branch[:, None, :]], axis=1).astype(jnp.float32)
    conv_out = jnp.sum(window * conv_taps.astype(jnp.float32)[None], axis=1)
    heads_here = w_recur.shape[0]
    head_width = w_recur.shape[1]
    conv_heads = conv_out.astype(jnp.bfloat16).reshape(seqs, heads_here, head_width)
    recur = jax.nn.sigmoid(
        jnp.einsum("nhi,hij->nhj", conv_heads, w_recur, preferred_element_type=jnp.float32).reshape(
            seqs, -1
        )
    )
    inject = jax.nn.sigmoid(
        jnp.einsum(
            "nhi,hij->nhj", conv_heads, w_inject, preferred_element_type=jnp.float32
        ).reshape(seqs, -1)
    )
    log_decay = -LRU_SCALE * recur * jax.nn.softplus(-lru_lambda)
    state_out = (
        jnp.exp(log_decay) * lru_state + jnp.sqrt(-jnp.expm1(2.0 * log_decay)) * inject * conv_out
    )
    lru_out = (state_out * jax.nn.gelu(gate_in.astype(jnp.float32))).astype(jnp.bfloat16)
    partial_value = jnp.dot(lru_out, w_out, preferred_element_type=jnp.float32)
    partial_value = lax.optimization_barrier(partial_value.astype(jnp.bfloat16)).astype(jnp.float32)
    mix_out = lax.psum_scatter(
        partial_value.astype(jnp.bfloat16), "tp", scatter_dimension=1, tiled=True
    )
    resid = (tokens.astype(jnp.float32) + mix_out.astype(jnp.float32)).astype(jnp.bfloat16)
    top = route_ids.shape[1]
    local = expert_gate.shape[0]
    experts = lax.axis_size("ep") * local
    capacity = max(2, 2 * seqs * top // experts)
    flat = route_ids.reshape(-1)
    onehot = (flat[:, None] == jnp.arange(experts, dtype=jnp.int32)[None, :]).astype(jnp.int32)
    before = jnp.cumsum(onehot, axis=0) - onehot
    slot = jnp.sum(before * onehot, axis=1)
    slot_id = slot * experts + flat
    places = jnp.arange(capacity * experts, dtype=jnp.int32)
    hits = slot_id[None, :] == places[:, None]
    dispatch = jnp.sum(
        hits.reshape(capacity * experts, seqs, top).astype(jnp.float32), axis=2
    ).astype(jnp.bfloat16)
    spread = jnp.transpose(hits).reshape(seqs, top, capacity * experts)
    combine = jnp.sum(jnp.where(spread, route_weight[:, :, None], 0.0), axis=1)
    values = resid.astype(jnp.float32)
    total = lax.psum(jnp.sum(values * values, axis=1), "tp")
    quarter = values.shape[1]
    start = lax.axis_index("tp") * quarter
    gain_here = lax.dynamic_slice_in_dim(ffn_gain, start, quarter, 0).astype(jnp.float32)
    scale = lax.rsqrt(total[:, None] / D + EPS)
    normed_part = (values * scale * gain_here).astype(jnp.bfloat16)
    buffer = jnp.dot(dispatch, normed_part, preferred_element_type=jnp.float32).astype(jnp.bfloat16)
    buffer = buffer.reshape(capacity, experts, -1)
    block = lax.all_gather(
        lax.all_to_all(buffer, "ep", split_axis=1, concat_axis=1, tiled=True),
        "tp",
        axis=2,
        tiled=True,
    )
    count = block.shape[0]
    width = block.shape[2]
    grid = block.reshape(count, -1, local, width)
    rows = grid[:, :, 0].reshape(-1, width)
    first = jnp.dot(rows, expert_gate[0], preferred_element_type=jnp.float32)
    second = jnp.dot(rows, expert_up[0], preferred_element_type=jnp.float32)
    hidden = (jax.nn.silu(first) * second).astype(jnp.bfloat16)
    term = jnp.dot(hidden, expert_down[0], preferred_element_type=jnp.float32)
    term = lax.optimization_barrier(term.astype(jnp.bfloat16)).astype(jnp.float32)
    summed = lax.psum_scatter(term.astype(jnp.bfloat16), "tp", scatter_dimension=1, tiled=True)
    results = summed.reshape(count, -1, 1, summed.shape[1])
    answered = results.reshape(count, -1, results.shape[3])
    returned = lax.all_to_all(answered, "ep", split_axis=1, concat_axis=1, tiled=True)
    back = returned.reshape(capacity * experts, -1).astype(jnp.float32)
    moe = jnp.dot(combine, back, precision=lax.Precision.HIGHEST)
    mixed = (resid.astype(jnp.float32) + moe).astype(jnp.bfloat16)
    return (mixed, state_out)


MESH = pl.DeviceIdType.MESH
F32 = jnp.float32
BF16 = jnp.bfloat16
GROUPS = 2


def kernel(
    ep_n,
    tp_n,
    cap,
    tokens,
    conv_state,
    lru_state,
    mix_gain,
    ffn_gain,
    w_branch,
    w_gate,
    conv_taps,
    w_recur,
    w_inject,
    lru_lambda,
    w_out,
    expert_gate,
    expert_up,
    expert_down,
    route_ids,
    route_weight,
    mixed_ref,
    state_ref,
    tok,
    v_conv,
    v_lru,
    v_mg,
    v_fg,
    v_wb,
    v_wg,
    v_taps,
    v_wr,
    v_wi,
    v_lam,
    v_wo,
    v_eg,
    v_eu,
    v_ed,
    v_ids,
    v_rw,
    mixs,
    mixr,
    dsend,
    xall,
    tsend,
    drx,
    esend,
    erx,
    rsend,
    ret,
    loc,
    s1,
    r1,
    s2,
    r2,
    s4,
    r4,
    sa,
    ra,
    sb,
    rb,
    sc,
    rc,
    sd,
    rd,
    se,
    re,
    sf,
    rf,
):
    e = lax.axis_index("ep")
    t = lax.axis_index("tp")
    half = t // 2
    core = t % 2
    partner = half * 2 + (1 - core)
    cross = (1 - half) * 2 + core
    diag = (1 - half) * 2 + (1 - core)
    peers = (diag, cross, partner)
    seqs, quarter = tokens.shape
    width = quarter * tp_n

    barrier = pltpu.get_barrier_semaphore()
    for k in range(1, ep_n):
        pl.semaphore_signal(
            barrier, inc=1, device_id=((e + k) % ep_n, t), device_id_type=MESH
        )
    for peer in peers:
        pl.semaphore_signal(barrier, inc=1, device_id=(e, peer), device_id_type=MESH)

    pairs = (
        (tokens, tok.at[t]),
        (mix_gain, v_mg),
        (w_branch, v_wb),
        (w_gate, v_wg),
        (conv_state, v_conv),
        (conv_taps, v_taps),
        (w_recur, v_wr),
        (w_inject, v_wi),
        (lru_lambda, v_lam),
        (lru_state, v_lru),
        (w_out, v_wo),
        (route_ids, v_ids),
        (route_weight, v_rw),
        (ffn_gain, v_fg),
        (expert_gate.at[0], v_eg),
        (expert_up.at[0], v_eu),
        (expert_down.at[0], v_ed),
    )
    loads = []
    for i, (source, target) in enumerate(pairs):
        load = pltpu.make_async_copy(source, target, loc.at[i])
        load.start()
        loads.append(load)

    sent = []

    def send(source, target, ssem, rsem, where):
        copy = pltpu.make_async_remote_copy(
            src_ref=source,
            dst_ref=target,
            send_sem=ssem,
            recv_sem=rsem,
            device_id=where,
            device_id_type=MESH,
        )
        copy.start()
        sent.append(copy)
        return copy

    loads[0].wait()
    pl.semaphore_wait(barrier, ep_n - 1 + tp_n - 1)

    gathers = [
        send(tok.at[t], tok.at[t], s1.at[j], r1.at[j], (e, peer)) for j, peer in enumerate(peers)
    ]

    loads[11].wait()
    loads[12].wait()
    ids = jnp.transpose(v_ids[...].astype(F32))
    lanes = lax.broadcasted_iota(jnp.int32, (seqs, 128), 1).astype(F32)
    hot0 = (lanes == ids[:, 0:1]).astype(F32)
    hot1 = (lanes == ids[:, 1:2]).astype(F32)
    lower = (
        lax.broadcasted_iota(jnp.int32, (seqs, seqs), 1)
        < lax.broadcasted_iota(jnp.int32, (seqs, seqs), 0)
    ).astype(F32).astype(BF16)
    before0 = jnp.dot(lower, hot0.astype(BF16), preferred_element_type=F32)
    before1 = jnp.dot(lower, hot1.astype(BF16), preferred_element_type=F32)
    before1 = before1 + jnp.sum(hot0, axis=0, keepdims=True)
    place0 = ids[:, 0:1] * cap + jnp.sum(before0 * hot0, axis=1, keepdims=True)
    place1 = ids[:, 1:2] * cap + jnp.sum(before1 * hot1, axis=1, keepdims=True)
    places = lax.broadcasted_iota(jnp.int32, (seqs, ep_n * cap), 1).astype(F32)
    hits0 = (places == place0).astype(F32)
    hits1 = (places == place1).astype(F32)
    dispatch = (hits0 + hits1).astype(BF16)
    hits0 = hits0.astype(BF16)
    hits1 = hits1.astype(BF16)

    for i in range(1, 11):
        loads[i].wait()
    convolved = jnp.zeros((seqs, v_taps.shape[1]), F32)
    taps = v_taps[...].astype(F32)
    steps = taps.shape[0]
    for j in range(steps - 1):
        convolved = convolved + v_conv[j].astype(F32) * taps[j : j + 1]
    soft = jnp.log1p(jnp.exp(-v_lam[...]))

    for copy in gathers:
        copy.wait_recv()
    whole = jnp.concatenate([tok[q] for q in range(tp_n)], axis=1).astype(F32)
    scale = lax.rsqrt(jnp.sum(whole * whole, axis=1, keepdims=True) / width + EPS)
    normed = (whole * scale * v_mg[...].astype(F32).reshape(1, width)).astype(BF16)
    branch = jnp.dot(normed, v_wb[...], preferred_element_type=F32).astype(BF16).astype(F32)
    gate_in = jnp.dot(normed, v_wg[...], preferred_element_type=F32).astype(BF16).astype(F32)
    conv_out = convolved + branch * taps[steps - 1 : steps]
    heads, head_w = w_recur.shape[0], w_recur.shape[1]
    rounded = conv_out.astype(BF16)
    pre_r, pre_i = [], []
    for h in range(heads):
        piece = rounded[:, h * head_w : (h + 1) * head_w]
        pre_r.append(jnp.dot(piece, v_wr[h], preferred_element_type=F32))
        pre_i.append(jnp.dot(piece, v_wi[h], preferred_element_type=F32))
    recur = jax.nn.sigmoid(jnp.concatenate(pre_r, axis=1))
    inject = jax.nn.sigmoid(jnp.concatenate(pre_i, axis=1))
    log_decay = -LRU_SCALE * recur * soft
    decay = jnp.exp(log_decay)
    kept = -jnp.tanh(log_decay) * (1.0 + decay * decay)
    state = decay * v_lru[...] + jnp.sqrt(kept) * inject * conv_out
    state_ref[...] = state
    lru_out = (state * jax.nn.gelu(gate_in)).astype(BF16)
    partial = jnp.dot(lru_out, v_wo[...], preferred_element_type=F32)
    for q in range(tp_n):
        mixs[q] = partial[:, q * quarter : (q + 1) * quarter].astype(BF16)

    parts = [
        send(mixs.at[peer], mixr.at[j], s2.at[j], r2.at[j], (e, peer))
        for j, peer in enumerate(peers)
    ]
    mix = mixs[t].astype(F32)
    for j, copy in enumerate(parts):
        copy.wait_recv()
        mix = mix + mixr[j].astype(F32)
    resid = (tok[t].astype(F32) + mix.astype(BF16).astype(F32)).astype(BF16)

    rows = lax.dot_general(
        dispatch, resid, (((0,), (0,)), ((), ())), preferred_element_type=F32
    ).astype(BF16)
    for p in range(ep_n):
        dsend[p] = rows[p * cap : (p + 1) * cap]
    near = sorted(range(1, ep_n), key=lambda k: min(k, ep_n - k))
    order = [0] + near
    arrivals = {}
    for k in reversed(near):
        there = (e + k) % ep_n
        arrivals[k] = send(dsend.at[there], xall.at[e, t], s4.at[k], r4.at[k], (there, t))
    xall[e, t] = dsend[e]

    aside, over, relayed = {}, {}, {}

    def relay(k):
        over[k].wait_recv()
        piece = xall.at[(e + ep_n - k) % ep_n, cross]
        relayed[k] = send(piece, piece, sc.at[k], rc.at[k], (e, partner))

    for k in order:
        if k:
            arrivals[k].wait_recv()
        own = dsend.at[e] if k == 0 else xall.at[(e + ep_n - k) % ep_n, t]
        slot = xall.at[(e + ep_n - k) % ep_n, t]
        over[k] = send(own, slot, sb.at[k], rb.at[k], (e, cross))
        aside[k] = send(own, slot, sa.at[k], ra.at[k], (e, partner))
    for k in order:
        relay(k)

    for i in range(13, 17):
        loads[i].wait()
    gain = v_fg[...].astype(F32).reshape(1, width)
    per = ep_n // GROUPS
    split = [order[g * per : (g + 1) * per] for g in range(GROUPS)]
    swaps = []
    for g in range(GROUPS):
        blocks = []
        for k in split[g]:
            aside[k].wait_recv()
            relayed[k].wait_recv()
            origin = (e + ep_n - k) % ep_n
            blocks.append(jnp.concatenate([xall[origin, q] for q in range(tp_n)], axis=1))
        block = jnp.concatenate(blocks, axis=0).astype(F32)
        scale = lax.rsqrt(jnp.sum(block * block, axis=1, keepdims=True) / width + EPS)
        normed2 = (block * scale * gain).astype(BF16)
        first = jnp.dot(normed2, v_eg[...], preferred_element_type=F32)
        second = jnp.dot(normed2, v_eu[...], preferred_element_type=F32)
        hidden = (jax.nn.silu(first) * second).astype(BF16)
        term = jnp.dot(hidden, v_ed[...], preferred_element_type=F32)
        for q in range(tp_n):
            tsend[g, q] = term[:, q * quarter : (q + 1) * quarter].astype(BF16)
        swaps.append(
            (
                send(tsend.at[g, diag], drx.at[g, 1], sd.at[g, 1], rd.at[g, 1], (e, partner)),
                send(tsend.at[g, partner], drx.at[g, 0], sd.at[g, 0], rd.at[g, 0], (e, partner)),
            )
        )

    crossed = []
    for g in range(GROUPS):
        swaps[g][0].wait_recv()
        esend[g] = (tsend[g, cross].astype(F32) + drx[g, 1].astype(F32)).astype(BF16)
        crossed.append(send(esend.at[g], erx.at[g], se.at[g], re.at[g], (e, cross)))

    returns = {}
    for g in range(GROUPS):
        swaps[g][1].wait_recv()
        mine = tsend[g, t].astype(F32) + drx[g, 0].astype(F32)
        crossed[g].wait_recv()
        answer = (mine + erx[g].astype(F32)).astype(BF16)
        for i, k in enumerate(split[g]):
            rsend[k] = answer[i * cap : (i + 1) * cap]
        for k in reversed(split[g]):
            if k == 0:
                ret[e] = rsend[0]
            else:
                there = (e + ep_n - k) % ep_n
                returns[k] = send(rsend.at[k], ret.at[e], sf.at[k], rf.at[k], (there, t))
    for k in near:
        returns[k].wait_recv()
    back = ret[...].reshape(ep_n * cap, quarter)
    weights = jnp.transpose(v_rw[...])
    moe = weights[:, 0:1] * jnp.dot(hits0, back, preferred_element_type=F32)
    moe = moe + weights[:, 1:2] * jnp.dot(hits1, back, preferred_element_type=F32)
    mixed_ref[...] = (resid.astype(F32) + moe).astype(BF16)
    for copy in sent:
        copy.wait_send()


LIMIT = 24 * 1024 * 1024


def finish(mixed_in, state_in, mixed_ref, state_ref):
    mixed_ref[...] = mixed_in[...]
    state_ref[...] = state_in[...]


def step(mesh, *args):
    ep_n, tp_n = mesh.shape["ep"], mesh.shape["tp"]
    tokens, route_ids, w_recur, expert_gate = args[0], args[15], args[8], args[12]
    seqs, quarter = tokens.shape
    top = route_ids.shape[1]
    local = expert_gate.shape[0]
    cap = max(2, 2 * seqs * top // (ep_n * local))
    if tp_n != 4 or local != 1 or top != 2 or cap % 16 or ep_n % GROUPS or ep_n > 128:
        return body(*args)
    args = list(args)
    args[1] = jnp.transpose(args[1], (1, 0, 2))
    args[10] = args[10].reshape(1, -1)
    args[15], args[16] = args[15].T, args[16].T
    args = [pltpu.with_memory_space_constraint(a, pltpu.HBM) for a in args]
    shapes = [a.shape for a in args]
    shapes[0] = (tp_n, seqs, quarter)
    for i in (12, 13, 14):
        shapes[i] = shapes[i][1:]
    buffers = [pltpu.VMEM(s, a.dtype) for s, a in zip(shapes, args)]
    group = cap * ep_n // GROUPS
    dma = pltpu.SemaphoreType.DMA
    buffers += [
        pltpu.VMEM((tp_n, seqs, quarter), BF16),
        pltpu.VMEM((tp_n - 1, seqs, quarter), BF16),
        pltpu.VMEM((ep_n, cap, quarter), BF16),
        pltpu.VMEM((ep_n, tp_n, cap, quarter), BF16),
        pltpu.VMEM((GROUPS, tp_n, group, quarter), BF16),
        pltpu.VMEM((GROUPS, 2, group, quarter), BF16),
        pltpu.VMEM((GROUPS, group, quarter), BF16),
        pltpu.VMEM((GROUPS, group, quarter), BF16),
        pltpu.VMEM((ep_n, cap, quarter), BF16),
        pltpu.VMEM((ep_n, cap, quarter), BF16),
        dma((len(args),)),
    ]
    counts = [(tp_n - 1,), (tp_n - 1,), (ep_n,), (ep_n,), (ep_n,), (ep_n,), (GROUPS, 2), (GROUPS,), (ep_n,)]
    for count in counts:
        buffers += [dma(count), dma(count)]
    mixed, state = pl.pallas_call(
        functools.partial(kernel, ep_n, tp_n, cap),
        out_shape=(
            jax.ShapeDtypeStruct((seqs, quarter), BF16),
            jax.ShapeDtypeStruct(args[2].shape, F32),
        ),
        in_specs=[pl.BlockSpec(memory_space=pltpu.HBM)] * len(args),
        out_specs=(pl.BlockSpec(memory_space=pltpu.VMEM), pl.BlockSpec(memory_space=pltpu.VMEM)),
        scratch_shapes=buffers,
        compiler_params=pltpu.CompilerParams(
            collective_id=0, has_side_effects=True, vmem_limit_bytes=LIMIT
        ),
    )(*args)
    return pl.pallas_call(
        finish,
        out_shape=(
            jax.ShapeDtypeStruct((seqs, quarter), BF16),
            jax.ShapeDtypeStruct(args[2].shape, F32),
        ),
        in_specs=[pl.BlockSpec(memory_space=pltpu.VMEM)] * 2,
        out_specs=(pl.BlockSpec(memory_space=pltpu.VMEM), pl.BlockSpec(memory_space=pltpu.VMEM)),
        compiler_params=pltpu.CompilerParams(vmem_limit_bytes=4 * 1024 * 1024),
    )(mixed, state)


def solution(mesh):
    placed = (
        P("ep", "tp"),
        P("ep", None, "tp"),
        P("ep", "tp"),
        P(),
        P(),
        P(None, "tp"),
        P(None, "tp"),
        P(None, "tp"),
        P("tp", None, None),
        P("tp", None, None),
        P("tp"),
        P("tp", None),
        P("ep", None, "tp"),
        P("ep", None, "tp"),
        P("ep", "tp", None),
        P("ep", None),
        P("ep", None),
    )
    return jax.shard_map(
        functools.partial(step, mesh), mesh=mesh, in_specs=placed, out_specs=(P("ep", "tp"), P("ep", "tp")), check_vma=False
    )
```
